32 devices in a mesh: ep: 16 (over z, y, x), tp: 2 (over core).
Axes of the slice: x: 2, y: 2, z: 4, core: 2. Of those that a mesh axis runs over, the one named last changes fastest.
Arguments:
- stream: bfloat16 [512, 2048], P('ep'), may hold values from -6 to 6
- mixer_gain: float32 [2048], replicated, may hold values from 0.1 to 1.9
- gate_proj: bfloat16 [2048, 1024], P(None, 'tp'), may hold values from -0.125 to 0.125
- input_proj: bfloat16 [2048, 1024], P(None, 'tp'), may hold values from -0.125 to 0.125
- state_maps: bfloat16 [2, 2048, 256], P(None, None, 'tp'), may hold values from -0.125 to 0.125
- step_proj: bfloat16 [2048, 16], P(None, 'tp'), may hold values from -0.125 to 0.125
- step_bias: float32 [16], P('tp'), may hold values from -3 to 0.5
- decay_rate: float32 [16], P('tp'), may hold values from 0.05 to 4
- input_taps: float32 [4, 1024], P(None, 'tp'), may hold values from -3 to 3
- map_taps: float32 [2, 4, 256], P(None, None, 'tp'), may hold values from -3 to 3
- input_past: bfloat16 [512, 3, 1024], P('ep', None, 'tp'), may hold values from -6 to 6
- map_past: bfloat16 [512, 2, 3, 256], P('ep', None, None, 'tp'), may hold values from -6 to 6
- head_state: float32 [512, 16, 4096], P('ep', 'tp'), may hold values from -1.6 to 1.6
- skip_gain: float32 [16], P('tp'), may hold values from 0 to 2
- inner_gain: float32 [1024], P('tp'), may hold values from 0.1 to 1.9
- mixer_out: bfloat16 [1024, 2048], P('tp'), may hold values from -0.1875 to 0.1875
- channel_gain: float32 [2048], replicated, may hold values from 0.1 to 1.9
- expert_ids: int32 [512, 2], P('ep'), may hold values from 0 to 7, all different within a row; in each aligned block of 32 rows (0 to 31, 32 to 63, ...) at most 12 rows name the same one
- expert_weight: float32 [512, 2], P('ep'), may hold values from 0.2 to 1
- expert_gate: bfloat16 [2048, 57344], P(None, ('ep', 'tp')), may hold values from -0.125 to 0.125
- expert_up: bfloat16 [2048, 57344], P(None, ('ep', 'tp')), may hold values from -0.125 to 0.125
- expert_down: bfloat16 [57344, 2048], P(('ep', 'tp')), may hold values from -0.0625 to 0.0625
- dense_gate: bfloat16 [2048, 5632], P('tp', 'ep'), may hold values from -0.125 to 0.125
- dense_up: bfloat16 [2048, 5632], P('tp', 'ep'), may hold values from -0.125 to 0.125
- dense_down: bfloat16 [5632, 2048], P('ep', 'tp'), may hold values from -0.078125 to 0.078125
- dense_mix: float32 [2048], P('tp'), may hold values from -2 to 2
Outputs:
- stream_out: bfloat16 [512, 2048], P('ep', 'tp')
- state_out: float32 [512, 16, 4096], P('ep', 'tp')
The draws below stay inside these ranges and needn't reach their ends.
Inputs may be any that keep to these rules, and one draw needn't show every extreme that they name: `expert_ids`: each row names 2 different experts. In each aligned block of 32 rows no expert is named by more than 12 rows, and in some block one expert is named by exactly 12 rows.
All inputs are finite; a program needn't handle non-finite values.
Results may differ from the reference program's by a relative error of at most 0.015.
Values may be sent and summed in bfloat16 or wider, within the bound.
A program may use at most 128 MiB of HBM per device.

```python
import math
import jax
import jax.numpy as jnp
import numpy as np
from jax import lax

D = 2048
INNER = 1024
HEAD = 64
HEADS = 16
GROUPS = 4
NSTATE = 64
CONV = 4
EXPERTS = 8
TOP_K = 2
EXPERT_HIDDEN = 7168
DENSE_HIDDEN = 5632
SEQ_DEV = 32
BATCH = 512
CAP = 12
N_EP = 16
N_TP = 2


def steps_of(stream_key, dims, shards, low, high):
    level = 1.0
    for dim, blocks in shards:
        heights = jax.random.uniform(jax.random.fold_in(jax.random.fold_in(stream_key, 6), dim), (blocks,), jnp.float32, low / len(shards), high / len(shards))
        level = level * jnp.repeat(jnp.exp(heights), dims[dim] // blocks).reshape((-1,) + (1,) * (len(dims) - 1 - dim))
    return level


def shared_out(stream_key, own, number, rows, amount, top, limit, skew):
    ranking = jax.random.permutation(stream_key, amount)
    packed, common = portions_of(amount, rows * top, limit, skew, True), portions_of(amount, rows * top, limit, skew, False)
    places = jnp.arange(amount)

    def named(sizes, turn):
        used = int((sizes > 0).sum())
        fixed = max(1, used // 4)
        passed = fixed + (places - fixed + turn * (used - fixed)) % max(1, amount - fixed)
        return jnp.zeros((amount,), jnp.int32).at[ranking[jnp.where(places < fixed, places, passed)]].set(jnp.asarray(sizes, jnp.int32))

    sizes = jnp.where(number % 4 == 0, named(packed, number // 4), named(common, number - number // 4 - 1))
    mixed = jax.random.permutation(jax.random.fold_in(own, 3), amount)
    source_of, taker = mixed[0:amount // 2 * 2:2], mixed[1:amount // 2 * 2:2]
    slack = jnp.minimum(sizes[source_of] - 1, limit - sizes[taker]) // 2
    slack = jnp.where((source_of == ranking[0]) | (taker == ranking[0]) | (sizes[taker] == 0), 0, jnp.maximum(slack, 0))
    passed = jax.random.randint(jax.random.fold_in(own, 4), (amount // 2,), 0, 1 << 20) % (slack + 1)
    sizes = sizes.at[source_of].add(-passed).at[taker].add(passed)
    items = jnp.searchsorted(jnp.cumsum(sizes), jnp.arange(rows * top), side="right").astype(jnp.int32)
    table = items.reshape(top, rows).T
    table = table[jax.random.permutation(jax.random.fold_in(own, 1), rows)]
    turn = jax.random.randint(jax.random.fold_in(own, 2), (rows, 1), 0, top)
    return jnp.take_along_axis(table, (jnp.arange(top)[None, :] + turn) % top, axis=1)


def portions_of(amount, total, most, skew, full):
    weights = [(1 << 20) // math.isqrt(rank ** skew) + 1 for rank in range(1, amount + 1)]
    largest = most if full else min(most, max(-(-total // amount), total * weights[0] // sum(weights)))
    least = 1 if total - largest >= amount - 1 else 0
    counts, rest = [largest] + [least] * (amount - 1), total - largest - least * (amount - 1)
    while rest > 0:
        free = [i for i in range(1, amount) if counts[i] < largest] or [i for i in range(1, amount) if counts[i] < most]
        whole, left = sum([weights[i] for i in free]), rest
        for i in free:
            extra = min(most - counts[i], max(1, left * weights[i] // whole), rest)
            counts[i] = counts[i] + extra
            rest = rest - extra
    return np.array(counts)


def noise(rng, shape, width, reach, pieces=(), kind=jnp.bfloat16):
    values = width * jax.random.normal(rng, shape, jnp.float32)
    if pieces:
        values = values * steps_of(rng, shape, pieces, -0.22, 0.18)
    return jnp.clip(values, -reach, reach).astype(kind)


def setup_inputs(seed: int = 0) -> dict:
    key_list = jax.random.split(jax.random.key(seed), 27)
    stream = noise(key_list[0], (BATCH, D), 1.0, 6.0, ((0, 16),))
    mixer_gain = jnp.clip(1.0 + 0.18 * jax.random.normal(key_list[1], (D,), jnp.float32), 0.1, 1.9)
    gate_proj = noise(key_list[2], (D, INNER), D ** -0.5, 0.125, ((1, 2),))
    input_proj = noise(key_list[3], (D, INNER), D ** -0.5, 0.125, ((1, 2),))
    state_maps = noise(key_list[4], (2, D, GROUPS * NSTATE), D ** -0.5, 0.125, ((2, 2),))
    step_proj = noise(key_list[5], (D, HEADS), D ** -0.5, 0.125, ((1, 2),))
    step_bias = jnp.clip(-3.0 + 3.5 * jax.random.uniform(key_list[6], (HEADS,), jnp.float32) ** steps_of(key_list[6], (HEADS,), ((0, 2),), -0.2, 0.2), -3.0, 0.5)
    decay_rate = jnp.clip(jnp.exp(math.log(4.0) - 4.3820266 * jax.random.uniform(key_list[7], (HEADS,), jnp.float32) ** steps_of(key_list[7], (HEADS,), ((0, 2),), -0.2, 0.2)), 0.05, 4.0)
    input_taps = noise(key_list[8], (CONV, INNER), 0.5, 3.0, ((1, 2),), jnp.float32)
    map_taps = noise(key_list[9], (2, CONV, GROUPS * NSTATE), 0.5, 3.0, ((2, 2),), jnp.float32)
    input_past = noise(key_list[10], (BATCH, CONV - 1, INNER), 1.0, 6.0, ((0, 16), (2, 2)))
    map_past = noise(key_list[11], (BATCH, 2, CONV - 1, GROUPS * NSTATE), 1.0, 6.0, ((0, 16), (3, 2)))
    head_state = noise(key_list[12], (BATCH, HEADS, HEAD * NSTATE), 0.2, 1.6, ((0, 16), (1, 2)), jnp.float32)
    skip_gain = jnp.clip(2.0 * jax.random.uniform(key_list[13], (HEADS,), jnp.float32) ** steps_of(key_list[13], (HEADS,), ((0, 2),), -0.2, 0.2), 0.0, 2.0)
    inner_gain = jnp.clip(1.0 + 0.18 * jax.random.normal(key_list[14], (INNER,), jnp.float32), 0.1, 1.9)
    mixer_out = noise(key_list[15], (INNER, D), INNER ** -0.5, 0.1875, ((0, 2),))
    channel_gain = jnp.clip(1.0 + 0.18 * jax.random.normal(key_list[16], (D,), jnp.float32), 0.1, 1.9)
    expert_ids_keys = jax.random.split(jax.random.fold_in(key_list[17], 1), BATCH // SEQ_DEV)
    expert_ids_turns = jax.random.permutation(jax.random.fold_in(key_list[17], 3), BATCH // SEQ_DEV)
    expert_ids = jax.vmap(lambda own, number: shared_out(jax.random.fold_in(key_list[17], 2), own, number, SEQ_DEV, EXPERTS, TOP_K, CAP, 2))(expert_ids_keys, expert_ids_turns).reshape((BATCH, TOP_K))
    expert_weight = jnp.clip(0.2 + 0.8 * jax.random.uniform(key_list[18], (BATCH, TOP_K), jnp.float32) ** steps_of(key_list[18], (BATCH, TOP_K), ((0, 16),), -0.2, 0.2), 0.2, 1.0)
    expert_gate = noise(key_list[19], (D, EXPERTS * EXPERT_HIDDEN), D ** -0.5, 0.125, ((1, 32),))
    expert_up = noise(key_list[20], (D, EXPERTS * EXPERT_HIDDEN), D ** -0.5, 0.125, ((1, 32),))
    expert_down = noise(key_list[21], (EXPERTS * EXPERT_HIDDEN, D), EXPERT_HIDDEN ** -0.5, 0.0625, ((0, 32),))
    dense_gate = noise(key_list[22], (D, DENSE_HIDDEN), D ** -0.5, 0.125, ((0, 2), (1, 16)))
    dense_up = noise(key_list[23], (D, DENSE_HIDDEN), D ** -0.5, 0.125, ((0, 2), (1, 16)))
    dense_down = noise(key_list[24], (DENSE_HIDDEN, D), DENSE_HIDDEN ** -0.5, 0.078125, ((0, 16), (1, 2)))
    dense_mix = jnp.clip(jax.random.uniform(key_list[25], (D,), jnp.float32, -2.0, 2.0) * steps_of(key_list[25], (D,), ((0, 2),), -0.4, 0.0), -2.0, 2.0)
    return {"stream": stream, "mixer_gain": mixer_gain, "gate_proj": gate_proj, "input_proj": input_proj, "state_maps": state_maps, "step_proj": step_proj, "step_bias": step_bias, "decay_rate": decay_rate, "input_taps": input_taps, "map_taps": map_taps, "input_past": input_past, "map_past": map_past, "head_state": head_state, "skip_gain": skip_gain, "inner_gain": inner_gain, "mixer_out": mixer_out, "channel_gain": channel_gain, "expert_ids": expert_ids, "expert_weight": expert_weight, "expert_gate": expert_gate, "expert_up": expert_up, "expert_down": expert_down, "dense_gate": dense_gate, "dense_up": dense_up, "dense_down": dense_down, "dense_mix": dense_mix}


EPS = 1e-06

def rms_scale(values):
    return values * lax.rsqrt(lax.optimization_barrier(jnp.mean(values * values, axis=-1, keepdims=True)) + EPS)

def short_conv(past_rows, newest, tap_weights, along):
    window = jnp.concatenate([past_rows, jnp.expand_dims(newest, along)], axis=along).astype(jnp.float32)
    return jax.nn.silu(lax.optimization_barrier(jnp.sum(window * tap_weights, axis=along)))

def mix_heads(stream, mixer_gain, gate_proj, input_proj, state_maps, step_proj, step_bias, decay_rate, input_taps, map_taps, input_past, map_past, head_state, skip_gain, inner_gain):
    row_count = stream.shape[0]
    normed = (rms_scale(stream.astype(jnp.float32)) * mixer_gain).astype(jnp.bfloat16)
    gate_in = jnp.dot(normed, gate_proj, preferred_element_type=jnp.float32).astype(jnp.bfloat16)
    input_new = jnp.dot(normed, input_proj, preferred_element_type=jnp.float32).astype(jnp.bfloat16)
    map_new = jnp.stack([jnp.dot(normed, state_maps[0], preferred_element_type=jnp.float32), jnp.dot(normed, state_maps[1], preferred_element_type=jnp.float32)], axis=1).astype(jnp.bfloat16)
    step_size = jax.nn.softplus(jnp.dot(normed, step_proj, preferred_element_type=jnp.float32) + step_bias)
    conv_in = short_conv(input_past, input_new, input_taps, 1)
    conv_map = short_conv(map_past, map_new, map_taps, 2)
    head_count = step_size.shape[1]
    per_group = HEADS // GROUPS
    group_count = head_count // per_group
    write_map = jnp.repeat(conv_map[:, 0].reshape(row_count, group_count, NSTATE), per_group, axis=1)
    read_map = jnp.repeat(conv_map[:, 1].reshape(row_count, group_count, NSTATE), per_group, axis=1)
    values = conv_in.reshape(row_count, head_count, HEAD)
    decay_now = jnp.exp(-decay_rate * step_size)
    state_old = head_state.reshape(row_count, head_count, HEAD, NSTATE)
    state_new = decay_now[:, :, None, None] * state_old + (step_size[:, :, None] * values)[:, :, :, None] * write_map[:, :, None, :]
    gated = lax.optimization_barrier(jnp.sum(state_new * read_map[:, :, None, :], axis=3)) + skip_gain[:, None] * values
    gated = gated.reshape(row_count, head_count * HEAD) * jax.nn.silu(gate_in.astype(jnp.float32))
    inner_out = rms_scale(gated.reshape(row_count, group_count, -1)).reshape(row_count, -1) * inner_gain
    return (inner_out.astype(jnp.bfloat16), state_new.reshape(row_count, head_count, HEAD * NSTATE))

def expert_sum(ffn_in, expert_ids, expert_weight, expert_gate, expert_up, expert_down):
    total_rows, feature_count = ffn_in.shape
    hidden = expert_gate.shape[1] // EXPERTS
    row_limit = min(total_rows, N_EP * CAP)

    def visit(running, expert_index):
        matched = expert_ids == expert_index
        chosen = jnp.any(matched, axis=1)
        weight = lax.optimization_barrier(jnp.sum(jnp.where(matched, expert_weight, jnp.zeros_like(expert_weight)), axis=1))
        picked = jnp.nonzero(chosen, size=row_limit, fill_value=0)[0].astype(jnp.int32)
        is_live = jnp.arange(row_limit, dtype=jnp.int32) < jnp.sum(chosen.astype(jnp.int32))
        taken_rows = ffn_in[picked]
        first_col = (expert_index * hidden).astype(jnp.int32)
        w_gate = lax.dynamic_slice_in_dim(expert_gate, first_col, hidden, 1)
        w_up = lax.dynamic_slice_in_dim(expert_up, first_col, hidden, 1)
        w_down = lax.dynamic_slice_in_dim(expert_down, first_col, hidden, 0)
        act = (jax.nn.silu(jnp.dot(taken_rows, w_gate, preferred_element_type=jnp.float32)) * jnp.dot(taken_rows, w_up, preferred_element_type=jnp.float32)).astype(jnp.bfloat16)
        result = jnp.dot(act, w_down, preferred_element_type=jnp.float32)
        scale = jnp.where(is_live, weight[picked], jnp.zeros_like(weight[picked]))
        return (running.at[picked].add(result * scale[:, None]), None)
    start_sum = jnp.zeros((total_rows, feature_count), jnp.float32)
    total, _ = lax.scan(visit, start_sum, jnp.arange(EXPERTS, dtype=jnp.int32))
    return total

def reference(stream, mixer_gain, gate_proj, input_proj, state_maps, step_proj, step_bias, decay_rate, input_taps, map_taps, input_past, map_past, head_state, skip_gain, inner_gain, mixer_out, channel_gain, expert_ids, expert_weight, expert_gate, expert_up, expert_down, dense_gate, dense_up, dense_down, dense_mix):
    inner_out, state_out = mix_heads(stream, mixer_gain, gate_proj, input_proj, state_maps, step_proj, step_bias, decay_rate, input_taps, map_taps, input_past, map_past, head_state, skip_gain, inner_gain)
    block_cols = inner_out.shape[1] // N_TP
    mixed = jnp.zeros((stream.shape[0], mixer_out.shape[1]), jnp.float32)
    for portion in range(N_TP):
        partial_out = jnp.dot(inner_out[:, portion * block_cols:(portion + 1) * block_cols], mixer_out[portion * block_cols:(portion + 1) * block_cols], preferred_element_type=jnp.float32)
        mixed = mixed + lax.optimization_barrier(partial_out.astype(jnp.bfloat16)).astype(jnp.float32)
    hidden_mid = stream.astype(jnp.float32) + mixed
    ffn_in = (rms_scale(hidden_mid) * channel_gain).astype(jnp.bfloat16)
    routed = expert_sum(ffn_in, expert_ids, expert_weight, expert_gate, expert_up, expert_down)
    dense_act = (jax.nn.silu(jnp.dot(ffn_in, dense_gate, preferred_element_type=jnp.float32)) * jnp.dot(ffn_in, dense_up, preferred_element_type=jnp.float32)).astype(jnp.bfloat16)
    dense_res = jnp.dot(dense_act, dense_down, preferred_element_type=jnp.float32)
    stream_out = (hidden_mid + routed + jax.nn.sigmoid(dense_mix) * dense_res).astype(jnp.bfloat16)
    return (stream_out, state_out)
```

```python
import functools

import jax
import jax.numpy as jnp
from jax import lax
from jax.experimental import pallas as pl
from jax.experimental.pallas import tpu as pltpu
from jax.sharding import PartitionSpec as P

HEAD = 64
HEADS = 16
GROUPS = 4
NSTATE = 64
EXPERTS = 8
TOP_K = 2
CAP = 12
PAST = 3

EPS = 1e-06
MESH = pl.DeviceIdType.MESH
TILE = 256
F32 = jnp.float32
BF16 = jnp.bfloat16
MAPS_LEFT = (((1,), (1,)), ((), ()))


def rms_scale(values):
    return values * lax.rsqrt(jnp.mean(values * values, axis=-1, keepdims=True) + EPS)


def silu(values):
    return values / (1.0 + jnp.exp(-values))


def f32_dot(left, right):
    return jnp.dot(left, right, preferred_element_type=F32)


def dot_by_rows(left, right):
    return lax.dot_general(left, right, MAPS_LEFT, preferred_element_type=F32)


def parts_of(value, count):
    parts = []
    for _ in range(count):
        part = value.astype(BF16)
        parts.append(part)
        value = value - part.astype(F32)
    return parts


def iota(shape, dim):
    return lax.broadcasted_iota(jnp.int32, shape, dim)


def grid_of(ep_count):
    side = 4 if ep_count % 64 == 0 else (2 if ep_count % 4 == 0 else 1)
    return side, ep_count // (side * side)


LOADS = 13


def mix_kernel(ep_count, step_bias, decay_rate, skip_gain, *refs):
    loads, refs = refs[:LOADS], refs[LOADS:]
    (state_in, inner_out, state_out, notes), refs = refs[:4], refs[4:]
    stores, refs = refs[:LOADS], refs[LOADS:]
    held, wide_fed, wide_write, wide_read, wide_decay, total, load_sem, in_sem, out_sem = refs
    copies = []
    for i, (src, dst) in enumerate(zip(loads, stores)):
        copies.append(pltpu.make_async_copy(src, dst, load_sem.at[i]))
        copies[-1].start()
    flat, lanes = held.shape
    tiles = lanes // TILE

    def stripe(t):
        return pl.ds(pl.multiple_of(t * TILE, TILE), TILE)

    for t in range(tiles):
        cut = stripe(t)
        pltpu.make_async_copy(state_in.at[:, cut], held.at[:, cut], in_sem.at[t]).start()

    (
        stream, mixer_gain, ids, weight, gate_proj, input_proj, state_maps, step_proj,
        input_taps, map_taps, input_past, map_past, inner_gain,
    ) = stores
    ready = iter(copies)

    def wait(count):
        for _ in range(count):
            next(ready).wait()

    wait(4)
    row_count = stream.shape[0]
    normed = (rms_scale(stream[...].astype(F32)) * mixer_gain[...]).astype(BF16)

    side, line = grid_of(ep_count)
    place_z = lax.axis_index("ep") // (side * side)
    span = notes.shape[2]
    expert = iota((EXPERTS, row_count), 0)
    named = [ids[k : k + 1, :] == expert for k in range(TOP_K)]
    hits = functools.reduce(jnp.logical_or, named)
    before = iota((row_count, row_count), 0) < iota((row_count, row_count), 1)
    rank = f32_dot(
        jnp.where(hits, 1.0, 0.0).astype(BF16), jnp.where(before, 1.0, 0.0).astype(BF16)
    )
    rank = jnp.where(hits, rank + 1.0, 0.0).astype(BF16)
    share = sum(jnp.where(named[k], weight[k : k + 1, :], 0.0) for k in range(TOP_K))
    lay = iota((row_count, span), 0) + place_z * row_count == iota((row_count, span), 1)
    lay = jnp.where(lay, 1.0, 0.0).astype(BF16)
    rank_out = f32_dot(rank, lay)
    share_out = sum(f32_dot(part, lay) for part in parts_of(share, 3)[::-1])
    for e in range(EXPERTS):
        notes[e, 0:1, :] = rank_out[e : e + 1, :]
        notes[e, 1:2, :] = share_out[e : e + 1, :]

    wait(4)
    gate_in = f32_dot(normed, gate_proj[...]).astype(BF16).astype(F32)
    input_new = f32_dot(normed, input_proj[...]).astype(BF16).astype(F32)
    map_new = [f32_dot(normed, state_maps[m]).astype(BF16).astype(F32) for m in range(2)]
    step = dot_by_rows(normed, step_proj[...])
    wait(5)
    channels = input_new.shape[1]
    conv_in = input_taps[PAST : PAST + 1, :] * input_new
    for t in range(PAST):
        conv_in = conv_in + input_taps[t : t + 1, :] * input_past[t].astype(F32)
    conv_in = silu(conv_in)
    olds = map_past.shape[0]
    sort_to = iota((olds, olds), 0)
    sort_from = iota((olds, olds), 1)
    source = (sort_to % row_count) * (2 * PAST) + sort_to // row_count
    sort = jnp.where(sort_from == source, 1.0, 0.0).astype(BF16)
    sorted_past = f32_dot(sort, map_past[...])
    conv_map = []
    for m in range(2):
        value = map_taps[m, PAST : PAST + 1, :] * map_new[m]
        for t in range(PAST):
            at = (t * 2 + m) * row_count
            value = value + map_taps[m, t : t + 1, :] * sorted_past[at : at + row_count]
        conv_map.append(silu(value))

    heads = flat // row_count
    per_group = HEADS // GROUPS

    def row_of(scalars, width):
        lane = iota((1, heads * width), 1) // width
        return sum(jnp.where(lane == h, scalars[h], 0.0) for h in range(heads))

    step = step + row_of(step_bias, 1)
    step_size = jnp.maximum(step, 0.0) + jnp.log1p(jnp.exp(-jnp.abs(step)))
    decay = jnp.exp(-row_of(decay_rate, 1) * step_size)

    def by_head(values):
        width = values.shape[1]
        wide = jnp.broadcast_to(values[:, None, :], (row_count, heads, width))
        return wide.reshape(flat, width)

    def column(values):
        hit = iota((flat, heads), 0) % heads == iota((flat, heads), 1)
        return jnp.sum(jnp.where(hit, by_head(values), 0.0), axis=1, keepdims=True)

    head = iota((flat, 2 * HEAD), 0) % heads
    half = iota((flat, 2 * HEAD), 1) // HEAD

    def doubled(values, which):
        pair = which // 2
        kept = values[:, : 2 * HEAD]
        for k in range(1, values.shape[1] // (2 * HEAD)):
            kept = jnp.where(pair == k, values[:, 2 * HEAD * k : 2 * HEAD * (k + 1)], kept)
        return jnp.where(half == which % 2, kept, pltpu.roll(kept, HEAD, 1))

    fed = column(step_size) * doubled(by_head(conv_in), head)
    high, middle, low = parts_of(fed, 3)
    zero = jnp.zeros_like(low)
    wide_fed[:, : 2 * HEAD] = jnp.where(half == 0, high, middle)
    wide_fed[:, 2 * HEAD :] = jnp.where(half == 0, low, zero)
    wide_write[...] = doubled(by_head(conv_map[0]), head // per_group)
    wide_read[...] = doubled(by_head(conv_map[1]), head // per_group)
    wide_decay[...] = jnp.broadcast_to(column(decay), wide_decay.shape)
    total[...] = jnp.zeros_like(total)
    repeat = TILE // (2 * HEAD)

    @pl.loop(0, tiles)
    def _(t):
        cut = stripe(t)
        shape = (4 * HEAD, TILE)
        base = t * (TILE // NSTATE)
        pick = iota(shape, 0) % HEAD == iota(shape, 1) // NSTATE + base
        pick = jnp.where(pick, 1.0, 0.0).astype(BF16)
        gather = iota((TILE, 2 * HEAD), 0) // NSTATE + base == iota((TILE, 2 * HEAD), 1) % HEAD
        gather = jnp.where(gather, 1.0, 0.0).astype(BF16)
        pltpu.make_async_copy(held.at[:, cut], held.at[:, cut], in_sem.at[t]).wait()
        spread = f32_dot(wide_fed[...], pick)
        write = jnp.concatenate([wide_write[...]] * repeat, axis=1)
        value = jnp.concatenate([wide_decay[...]] * repeat, axis=1) * held[:, cut]
        value = value + spread * write
        held[:, cut] = value
        pltpu.make_async_copy(held.at[:, cut], state_out.at[:, cut], out_sem.at[t]).start()
        product = value * jnp.concatenate([wide_read[...]] * repeat, axis=1)
        total[...] += sum(f32_dot(part, gather) for part in parts_of(product, 2)[::-1])

    pieces = []
    for k in range(channels // (2 * HEAD)):
        mine = (head // 2 == k) & (half == head % 2)
        piece = jnp.where(mine, total[...], 0.0).reshape(row_count, heads, 2 * HEAD)
        pieces.append(jnp.sum(piece, axis=1))
    gated = jnp.concatenate(pieces, axis=1) + row_of(skip_gain, HEAD) * conv_in
    gated = gated * silu(gate_in)
    group = per_group * HEAD
    for at in range(0, channels, group):
        cut = slice(at, at + group)
        scaled = rms_scale(gated[:, cut]) * inner_gain[:, cut]
        inner_out[:, cut] = scaled.astype(BF16)
    for t in range(tiles):
        cut = stripe(t)
        pltpu.make_async_copy(held.at[:, cut], state_out.at[:, cut], out_sem.at[t]).wait()


def mix_heads(
    stream, mixer_gain, gate_proj, input_proj, state_maps, step_proj, step_bias, decay_rate,
    input_taps, map_taps, input_past, map_past, head_state, skip_gain, inner_gain,
    expert_ids, expert_weight,
):
    ep_count = lax.axis_size("ep")
    side, line = grid_of(ep_count)
    row_count = stream.shape[0]
    heads, lanes = head_state.shape[1:]
    channels = gate_proj.shape[1]
    flat = row_count * heads
    loads = (
        stream, mixer_gain[None, :], expert_ids.T, expert_weight.T,
        gate_proj, input_proj, state_maps, step_proj.T,
        input_taps, map_taps, input_past.transpose(1, 0, 2),
        map_past.transpose(0, 2, 1, 3).reshape(-1, map_past.shape[3]), inner_gain[None, :],
    )
    vmem = pl.BlockSpec(memory_space=pltpu.VMEM)
    smem = pl.BlockSpec(memory_space=pltpu.SMEM)
    any_space = pl.BlockSpec(memory_space=pl.ANY)
    dma = pltpu.SemaphoreType.DMA
    wide = pltpu.VMEM((flat, 2 * HEAD), F32)
    inner, state_new, notes = pl.pallas_call(
        functools.partial(mix_kernel, ep_count),
        out_shape=(
            jax.ShapeDtypeStruct((row_count, channels), BF16),
            jax.ShapeDtypeStruct((flat, lanes), F32),
            jax.ShapeDtypeStruct((EXPERTS, 2, line * row_count), F32),
        ),
        in_specs=[smem] * 3 + [any_space] * (LOADS + 1),
        out_specs=(vmem, any_space, vmem),
        scratch_shapes=[pltpu.VMEM(x.shape, x.dtype) for x in loads] + [
            pltpu.VMEM((flat, lanes), F32),
            pltpu.VMEM((flat, 4 * HEAD), BF16),
            wide, wide, wide, wide,
            dma((LOADS,)), dma((lanes // TILE,)), dma((lanes // TILE,)),
        ],
        compiler_params=pltpu.CompilerParams(vmem_limit_bytes=60 * 1024 * 1024),
        name="mix",
    )(step_bias, decay_rate, skip_gain, *loads, head_state.reshape(flat, lanes))
    return inner, state_new.reshape(row_count, heads, lanes), notes


class Place:
    def __init__(self, ep_count):
        self.side, self.line = grid_of(ep_count)
        self.ep = lax.axis_index("ep")
        self.core = lax.axis_index("tp")
        self.col = self.ep % self.side
        self.row = (self.ep // self.side) % self.side
        self.z = self.ep // (self.side * self.side)

    def ahead(self, db, da, core=None):
        core = self.core if core is None else core
        a = (self.row * (1 - core) + self.col * core + da) % self.side
        b = (self.col * (1 - core) + self.row * core + db) % self.side
        return a * (1 - core) + b * core, b * (1 - core) + a * core

    def near(self, db, da, dz):
        row, col = self.ahead(db, da)
        z = (self.z + dz) % self.line
        return {"ep": (z * self.side + row) * self.side + col, "tp": self.core}

    def plane(self, db, da):
        row, col = self.ahead(db, da)
        return row * self.side + col

    def spot(self, db, da, dz):
        return self.plane(db, da) * self.line + (self.z + dz) % self.line

    def sibling(self):
        return {"ep": self.ep, "tp": 1 - self.core}

    def z_order(self):
        line = self.line
        return sorted(range(1, line), key=lambda d: (min(d, line - d), d))


def greet(targets):
    barrier = pltpu.get_barrier_semaphore()
    for target in targets:
        pl.semaphore_signal(barrier, inc=1, device_id=target, device_id_type=MESH)
    return lambda: pl.semaphore_wait(barrier, len(targets))


def ffn_kernel(ep_count, *refs):
    (
        inner, stream, gain, notes_in, mix, mixer_out, dense_gate, dense_up, dense_down,
        expert_gate, expert_up, expert_down, out,
        out_w, gate_w, up_w, down_w, wide_gate, wide_up, wide_down,
        partial, other, hidden, every, notes, acts, rows, act, dense, own, give, take, share,
        total, from_b, from_a, from_z,
        load_sem, swap_sem, note_send, note_recv, link_send, link_recv, core_send, core_recv,
        weight_sem, act_send, act_recv, give_sem, sum_send, recv_b, recv_a, recv_z,
    ) = refs
    place = Place(ep_count)
    side, line = place.side, place.line
    core, me = place.core, place.ep
    row_count, width = stream.shape
    half = width // 2
    units = dense_gate.shape[0]
    part = row_count // 2
    span = line * row_count
    slots = line * CAP
    my_rows = pl.ds(pl.multiple_of(core * part, part), part)
    my_half = pl.ds(pl.multiple_of(core * half, half), half)
    everyone = [{"ep": (me + d) % ep_count, "tp": core} for d in range(1, ep_count)]
    greeted = greet([place.sibling()] + everyone)
    sends = []

    def load(at, src, dst):
        copy = pltpu.make_async_copy(src, dst, load_sem.at[at])
        copy.start()
        return copy

    def send(src, dst, send_sem, recv_sem, target):
        copy = pltpu.make_async_remote_copy(
            src_ref=src, dst_ref=dst, send_sem=send_sem, recv_sem=recv_sem,
            device_id=target, device_id_type=MESH,
        )
        copy.start()
        sends.append(copy)
        return copy

    def landed(ref, sem):
        pltpu.make_async_copy(ref, ref, sem).wait()

    out_load = load(0, mixer_out, out_w)
    dense_loads = [
        load(1, dense_gate, gate_w.at[core]),
        load(2, dense_up, up_w.at[core]),
        load(3, dense_down, down_w),
    ]
    out_load.wait()
    partial[...] = f32_dot(inner[...], out_w[...]).astype(BF16)
    expert_loads = [
        load(4, expert_gate, wide_gate), load(5, expert_up, wide_up),
        load(6, expert_down, wide_down),
    ]
    greeted()
    swap = send(partial, other, swap_sem.at[0], swap_sem.at[1], place.sibling())
    here = place.spot(0, 0, 0)
    for d in range(1, ep_count):
        target = (me + d) % ep_count
        expert = target // (ep_count // EXPERTS)
        send(
            notes_in.at[expert], notes.at[here], note_send.at[d - 1], note_recv.at[d - 1],
            everyone[d - 1],
        )
    notes[here] = notes_in[me // (ep_count // EXPERTS)]
    swap.wait_recv()
    middle = stream[...].astype(F32) + (partial[...].astype(F32) + other[...].astype(F32))
    hidden[...] = middle
    every[here] = (rms_scale(middle) * gain[...]).astype(BF16)

    def slot(db, da, dz):
        return ((db % side) * side + da % side) * line + dz % line

    def block(off):
        return every.at[place.spot(*off), my_rows]

    used = [0]

    def pass_on(off, step):
        there = slot(*(o - s for o, s in zip(off, step)))
        send(
            block(off), block(off), link_send.at[used[0]], link_recv.at[there], place.near(*step)
        )
        used[0] += 1

    def arrived(off):
        at = slot(*off)
        landed(block(off), link_recv.at[at])
        send(block(off), block(off), core_send.at[at], core_recv.at[at], place.sibling())

    zs = [0] + place.z_order()
    for dz in zs[1:]:
        pass_on((0, 0, 0), (0, 0, dz))
    for i, (src, dst) in enumerate(((dense_gate, gate_w), (dense_up, up_w))):
        send(
            src, dst.at[core], weight_sem.at[2 * i], weight_sem.at[2 * i + 1], place.sibling()
        )
    for dz in zs:
        if dz:
            arrived((0, 0, dz))
        for d in range(1, side):
            pass_on((0, 0, dz), (0, d, 0))
        for d in range(1, side):
            pass_on((0, 0, dz), (d, 0, 0))
    for dz in zs:
        for da in range(1, side):
            arrived((0, da, dz))
            for d in range(1, side):
                pass_on((0, da, dz), (d, 0, 0))

    def planes_of(db):
        return [(db, da) for da in range(side)]

    def group(at, size):
        return pl.ds(pl.multiple_of(at * size, size), size)

    for i, dst in enumerate((gate_w, up_w)):
        dense_loads[i].wait()
        landed(dst.at[1 - core], weight_sem.at[2 * i + 1])

    def dense_in(planes):
        tall = len(planes) * line * part
        seen = jnp.concatenate(
            [every[group(place.plane(*at), line), my_rows].reshape(-1, width) for at in planes],
            axis=0,
        )

        def product(weights):
            return dot_by_rows(seen[:, :half], weights[0]) + dot_by_rows(
                seen[:, half:], weights[1]
            )

        value = (silu(product(gate_w)) * product(up_w)).astype(BF16)
        value = value.reshape(len(planes), line, part, units)
        for i, at in enumerate(planes):
            theirs = acts.at[group(place.plane(*at), line), my_rows]
            acts[group(place.plane(*at), line), my_rows] = value[i]
            k = at[0] * side + at[1]
            send(theirs, theirs, act_send.at[k], act_recv.at[k], place.sibling())

    dense_in(planes_of(0))
    for dz in zs:
        for da in range(side):
            for db in range(1, side):
                arrived((db, da, dz))
    for db in range(1, side):
        dense_in(planes_of(db))
    for d in range(1, ep_count):
        source = (me + ep_count - d) % ep_count
        at = (source % (side * side)) * line + source // (side * side)
        landed(notes.at[at], note_recv.at[d - 1])

    def matches(at):
        info = notes[group(at, line)].sum(axis=0)
        slot_id = iota((slots, span), 0)
        row_id = iota((slots, span), 1)
        hit = (slot_id // CAP == row_id // row_count) & (
            (slot_id % CAP + 1).astype(F32) == info[0:1]
        )
        return hit, info[1:2]

    planes = [(db, da) for db in range(side) for da in range(side)]
    for db, da in planes:
        at = place.plane(db, da)
        for dz in zs:
            if db or da or dz:
                theirs = every.at[place.spot(db, da, dz), other_rows(core, part)]
                landed(theirs, core_recv.at[slot(da, db, dz)])
        hit, _ = matches(at)
        pick = jnp.where(hit, 1.0, 0.0).astype(BF16)
        seen = every[group(at, line)].reshape(span, width)
        rows[group(at, slots), :] = f32_dot(pick, seen).astype(BF16)

    for copy in expert_loads:
        copy.wait()
    deep = expert_gate.shape[1]
    for at in range(0, deep, TILE):
        cut = slice(at, min(at + TILE, deep))
        gated = silu(f32_dot(rows[...], wide_gate[:, cut]))
        act[:, cut] = (gated * f32_dot(rows[...], wide_up[:, cut])).astype(BF16)
    scale = []
    for at in range(side * side):
        hit, weight = matches(at)
        scale.append(jnp.sum(jnp.where(hit, weight, 0.0), axis=1, keepdims=True))
    scale = jnp.concatenate(scale, axis=0)

    def results(first, at):
        cut = pl.ds(pl.multiple_of(first * half + at, TILE), TILE)
        return f32_dot(act[...], wide_down[:, cut]) * scale

    for at in range(0, half, TILE):
        give[:, at : at + TILE] = results(1 - core, at).astype(BF16)
    send(give, take, give_sem.at[0], give_sem.at[1], place.sibling())
    for at in range(0, half, TILE):
        own[:, at : at + TILE] = results(core, at)

    dense_loads[2].wait()
    mixed = jax.nn.sigmoid(mix[...])

    def dense_out(db, da):
        at = place.plane(db, da)
        theirs = acts.at[group(at, line), other_rows(core, part)]
        landed(theirs, act_recv.at[da * side + db])
        seen = acts[group(at, line)].reshape(span, units)
        dense[group(at, span), :] = f32_dot(seen, down_w[...]) * mixed

    for db in range(1, side):
        for da in range(side):
            dense_out(db, da)
    landed(take, give_sem.at[1])
    share[...] = (own[...] + take[...].astype(F32)).astype(BF16)

    def result(db, da):
        at = place.plane(db, da)
        hit, _ = matches(at)
        pick = jnp.where(hit, 1.0, 0.0).T.astype(BF16)
        back = f32_dot(pick, share[group(at, slots), :])
        dense[group(at, span), :] = dense[group(at, span), :] + back

    order = place.z_order() + [0]
    used[0] = 0

    def block_of(off):
        return dense[group(place.spot(*off), row_count), :]

    def give_to(value, dst, sem, step):
        at = used[0]
        used[0] += 1
        total[at] = value.astype(BF16)
        send(total.at[at], dst, sum_send.at[at], sem, place.near(*step))

    def add(value, ref, sem):
        landed(ref, sem)
        return value + ref[...].astype(F32)

    for da in list(range(1, side)) + [0]:
        for db in range(1, side):
            result(db, da)
            for dz in order:
                give_to(
                    block_of((db, da, dz)), from_b.at[db - 1, da, dz], recv_b.at[db - 1, da, dz],
                    (db, 0, 0),
                )
    for da in list(range(1, side)) + [0]:
        dense_out(0, da)
        result(0, da)
        for dz in order:
            value = block_of((0, da, dz))
            for d in range(1, side):
                value = add(value, from_b.at[d - 1, da, dz], recv_b.at[d - 1, da, dz])
            if da:
                give_to(value, from_a.at[da - 1, dz], recv_a.at[da - 1, dz], (0, da, 0))
                continue
            for d in range(1, side):
                value = add(value, from_a.at[d - 1, dz], recv_a.at[d - 1, dz])
            if dz:
                give_to(value, from_z.at[dz - 1], recv_z.at[dz - 1], (0, 0, dz))
                continue
            for d in range(1, line):
                value = add(value, from_z.at[d - 1], recv_z.at[d - 1])
            out[...] = (hidden[:, my_half] + value).astype(out.dtype)
    for copy in sends:
        copy.wait_send()


def other_rows(core, part):
    return pl.ds(pl.multiple_of((1 - core) * part, part), part)


def ffn(
    inner, stream, gain, notes, mix, mixer_out, dense_gate, dense_up, dense_down,
    expert_gate, expert_up, expert_down,
):
    ep_count = lax.axis_size("ep")
    side, line = grid_of(ep_count)
    row_count, width = stream.shape
    half = width // 2
    units = dense_gate.shape[0]
    deep = expert_gate.shape[1]
    slots = ep_count * CAP
    more = max(side - 1, 1)
    block = (row_count, half)
    vmem = pl.BlockSpec(memory_space=pltpu.VMEM)
    any_space = pl.BlockSpec(memory_space=pl.ANY)
    dma = pltpu.SemaphoreType.DMA

    def half_words(*shape):
        return pltpu.VMEM(shape, BF16)

    def words(*shape):
        return pltpu.VMEM(shape, F32)

    return pl.pallas_call(
        functools.partial(ffn_kernel, ep_count),
        out_shape=jax.ShapeDtypeStruct(block, BF16),
        in_specs=[vmem] * 5 + [any_space] * 7,
        out_specs=vmem,
        scratch_shapes=[
            half_words(*mixer_out.shape),
            half_words(2, units, half), half_words(2, units, half), half_words(units, half),
            half_words(width, deep), half_words(width, deep), half_words(deep, width),
            half_words(row_count, width), half_words(row_count, width), words(row_count, width),
            half_words(ep_count, row_count, width), words((ep_count), *notes.shape[1:]),
            half_words(ep_count, row_count, units),
            half_words(slots, width), half_words(slots, deep),
            words(ep_count * row_count, half),
            words(slots, half), half_words(slots, half), half_words(slots, half),
            half_words(slots, half),
            half_words(ep_count, *block), half_words(more, side, line, *block),
            half_words(more, line, *block), half_words(max(line - 1, 1), *block),
            dma((7,)), dma((2,)), dma((ep_count,)), dma((ep_count,)),
            dma((ep_count,)), dma((ep_count,)), dma((ep_count,)), dma((ep_count,)),
            dma((4,)), dma((side * side,)), dma((side * side,)), dma((2,)),
            dma((ep_count,)), dma((more, side, line)), dma((more, line)),
            dma((max(line - 1, 1),)),
        ],
        compiler_params=pltpu.CompilerParams(
            collective_id=1, has_side_effects=True, vmem_limit_bytes=60 * 1024 * 1024
        ),
        name="ffn",
    )(
        inner, stream, gain, notes, mix, mixer_out, dense_gate, dense_up, dense_down,
        expert_gate, expert_up, expert_down,
    )


def local(
    stream, mixer_gain, gate_proj, input_proj, state_maps, step_proj, step_bias, decay_rate,
    input_taps, map_taps, input_past, map_past, head_state, skip_gain, inner_gain, mixer_out,
    channel_gain, expert_ids, expert_weight, expert_gate, expert_up, expert_down,
    dense_gate, dense_up, dense_down, dense_mix,
):
    inner, state_out, notes = mix_heads(
        stream, mixer_gain, gate_proj, input_proj, state_maps, step_proj, step_bias, decay_rate,
        input_taps, map_taps, input_past, map_past, head_state, skip_gain, inner_gain,
        expert_ids, expert_weight,
    )
    updated = ffn(
        inner, stream, channel_gain[None, :], notes, dense_mix[None, :], mixer_out,
        dense_gate.T, dense_up.T, dense_down, expert_gate, expert_up, expert_down,
    )
    return (updated, state_out)


def solution(mesh):
    placed = (
        P("ep", None),
        P(),
        P(None, "tp"),
        P(None, "tp"),
        P(None, None, "tp"),
        P(None, "tp"),
        P("tp"),
        P("tp"),
        P(None, "tp"),
        P(None, None, "tp"),
        P("ep", None, "tp"),
        P("ep", None, None, "tp"),
        P("ep", "tp", None),
        P("tp"),
        P("tp"),
        P("tp", None),
        P(),
        P("ep", None),
        P("ep", None),
        P(None, ("ep", "tp")),
        P(None, ("ep", "tp")),
        P(("ep", "tp"), None),
        P("tp", "ep"),
        P("tp", "ep"),
        P("ep", "tp"),
        P("tp"),
    )
    return jax.shard_map(
        local,
        mesh=mesh,
        in_specs=placed,
        out_specs=(P("ep", "tp"), P("ep", "tp", None)),
        check_vma=False,
    )
```

```python
import functools

import jax
import jax.numpy as jnp
from jax import lax
from jax.experimental import pallas as pl
from jax.experimental.pallas import tpu as pltpu
from jax.sharding import PartitionSpec as P

HEAD = 64
HEADS = 16
GROUPS = 4
NSTATE = 64
EXPERTS = 8
TOP_K = 2
CAP = 12
PAST = 3

EPS = 1e-06
MESH = pl.DeviceIdType.MESH
TILE = 256
STRAIGHT_OUT = 1
STRAIGHT_BACK = 1
CHUNK = 4 * TILE
F32 = jnp.float32
BF16 = jnp.bfloat16
MAPS_LEFT = (((1,), (1,)), ((), ()))


def rms_scale(values):
    return values * lax.rsqrt(jnp.mean(values * values, axis=-1, keepdims=True) + EPS)


def silu(values):
    return values / (1.0 + jnp.exp(-values))


def f32_dot(left, right):
    return jnp.dot(left, right, preferred_element_type=F32)


def dot_by_rows(left, right):
    return lax.dot_general(left, right, MAPS_LEFT, preferred_element_type=F32)


def parts_of(value, count):
    parts = []
    for _ in range(count):
        part = value.astype(BF16)
        parts.append(part)
        value = value - part.astype(F32)
    return parts


def iota(shape, dim):
    return lax.broadcasted_iota(jnp.int32, shape, dim)


def grid_of(ep_count):
    side = 4 if ep_count % 64 == 0 else (2 if ep_count % 4 == 0 else 1)
    return side, ep_count // (side * side)


LOADS = 14


def mix_kernel(step_bias, decay_rate, skip_gain, *refs):
    loads, refs = refs[:LOADS], refs[LOADS:]
    (state_in, partial, state_out, note), refs = refs[:4], refs[4:]
    stores, refs = refs[:LOADS], refs[LOADS:]
    inner, held, wide_fed, wide_write, wide_read, wide_decay, total = refs[:7]
    picks, gathers, load_sem, in_sem, out_sem = refs[7:]
    copies = []
    for i, (src, dst) in enumerate(zip(loads, stores)):
        copies.append(pltpu.make_async_copy(src, dst, load_sem.at[i]))
        if i < LOADS - 1:
            copies[-1].start()
    flat, lanes = held.shape
    tiles = lanes // TILE

    def stripe(t):
        return pl.ds(pl.multiple_of(t * TILE, TILE), TILE)

    def chunk(c):
        return pl.ds(pl.multiple_of(c * CHUNK, CHUNK), CHUNK)

    @pl.loop(0, tiles)
    def _(t):
        base = t * (TILE // NSTATE)
        shape = (4 * HEAD, TILE)
        pick = iota(shape, 0) % HEAD - iota(shape, 1) // NSTATE == base
        picks[:, stripe(t)] = jnp.where(pick, 1.0, 0.0).astype(BF16)
        shape = (TILE, 2 * HEAD)
        gather = iota(shape, 1) % HEAD - iota(shape, 0) // NSTATE == base
        gathers[stripe(t), :] = jnp.where(gather, 1.0, 0.0)

    (
        stream, mixer_gain, ids, weight, gate_proj, input_proj, state_maps, step_proj,
        input_taps, map_taps, input_past, map_past, inner_gain, mixer_out,
    ) = stores
    ready = iter(copies)

    def wait(count):
        for _ in range(count):
            next(ready).wait()

    wait(4)
    for c in range(lanes // CHUNK):
        pltpu.make_async_copy(state_in.at[:, chunk(c)], held.at[:, chunk(c)], in_sem.at[c]).start()
    copies[-1].start()
    row_count = stream.shape[0]
    normed = (rms_scale(stream[...].astype(F32)) * mixer_gain[...]).astype(BF16)

    note[...] = jnp.zeros_like(note)
    note[:TOP_K, :row_count] = weight[...]
    note[TOP_K:, :row_count] = ids[...].astype(F32)

    wait(4)
    gate_in = f32_dot(normed, gate_proj[...]).astype(BF16).astype(F32)
    input_new = f32_dot(normed, input_proj[...]).astype(BF16).astype(F32)
    map_new = [f32_dot(normed, state_maps[m]).astype(BF16).astype(F32) for m in range(2)]
    step = dot_by_rows(normed, step_proj[...])
    wait(5)
    channels = input_new.shape[1]
    conv_in = input_taps[PAST : PAST + 1, :] * input_new
    for t in range(PAST):
        conv_in = conv_in + input_taps[t : t + 1, :] * input_past[t].astype(F32)
    conv_in = silu(conv_in)
    olds = map_past.shape[0]
    sort_to = iota((olds, olds), 0)
    sort_from = iota((olds, olds), 1)
    source = (sort_to % row_count) * (2 * PAST) + sort_to // row_count
    sort = jnp.where(sort_from == source, 1.0, 0.0).astype(BF16)
    sorted_past = f32_dot(sort, map_past[...])
    conv_map = []
    for m in range(2):
        value = map_taps[m, PAST : PAST + 1, :] * map_new[m]
        for t in range(PAST):
            at = (t * 2 + m) * row_count
            value = value + map_taps[m, t : t + 1, :] * sorted_past[at : at + row_count]
        conv_map.append(silu(value))

    heads = flat // row_count
    per_group = HEADS // GROUPS

    def row_of(scalars, width):
        lane = iota((1, heads * width), 1) // width
        return sum(jnp.where(lane == h, scalars[h], 0.0) for h in range(heads))

    step = step + row_of(step_bias, 1)
    step_size = jnp.maximum(step, 0.0) + jnp.log1p(jnp.exp(-jnp.abs(step)))
    decay = jnp.exp(-row_of(decay_rate, 1) * step_size)

    def by_head(values):
        width = values.shape[1]
        wide = jnp.broadcast_to(values[:, None, :], (row_count, heads, width))
        return wide.reshape(flat, width)

    def column(values):
        hit = iota((flat, heads), 0) % heads == iota((flat, heads), 1)
        return jnp.sum(jnp.where(hit, by_head(values), 0.0), axis=1, keepdims=True)

    head = iota((flat, 2 * HEAD), 0) % heads
    half = iota((flat, 2 * HEAD), 1) // HEAD

    def doubled(values, which):
        pair = which // 2
        kept = values[:, : 2 * HEAD]
        for k in range(1, values.shape[1] // (2 * HEAD)):
            kept = jnp.where(pair == k, values[:, 2 * HEAD * k : 2 * HEAD * (k + 1)], kept)
        return jnp.where(half == which % 2, kept, pltpu.roll(kept, HEAD, 1))

    fed = column(step_size) * doubled(by_head(conv_in), head)
    high, middle, low = parts_of(fed, 3)
    zero = jnp.zeros_like(low)
    wide_fed[:, : 2 * HEAD] = jnp.where(half == 0, high, middle)
    wide_fed[:, 2 * HEAD :] = jnp.where(half == 0, low, zero)
    wide_write[...] = doubled(by_head(conv_map[0]), head // per_group)
    wide_read[...] = doubled(by_head(conv_map[1]), head // per_group)
    wide_decay[...] = jnp.broadcast_to(column(decay), wide_decay.shape)
    repeat = TILE // (2 * HEAD)

    write = jnp.concatenate([wide_write[...]] * repeat, axis=1)
    read = jnp.concatenate([wide_read[...]] * repeat, axis=1)
    decay_now = jnp.concatenate([wide_decay[...]] * repeat, axis=1)
    sums = []
    for c in range(lanes // CHUNK):
        cut = chunk(c)
        pltpu.make_async_copy(held.at[:, cut], held.at[:, cut], in_sem.at[c]).wait()
        for at in range(c * CHUNK, (c + 1) * CHUNK, TILE):
            at = slice(at, at + TILE)
            value = decay_now * held[:, at] + f32_dot(wide_fed[...], picks[:, at]) * write
            held[:, at] = value
            sums.append(f32_dot(value * read, gathers[at]))
        pltpu.make_async_copy(held.at[:, cut], state_out.at[:, cut], out_sem.at[c]).start()
    total[...] = sum(sums)

    pieces = []
    for k in range(channels // (2 * HEAD)):
        mine = (head // 2 == k) & (half == head % 2)
        piece = jnp.where(mine, total[...], 0.0).reshape(row_count, heads, 2 * HEAD)
        pieces.append(jnp.sum(piece, axis=1))
    gated = jnp.concatenate(pieces, axis=1) + row_of(skip_gain, HEAD) * conv_in
    gated = gated * silu(gate_in)
    group = per_group * HEAD
    for at in range(0, channels, group):
        cut = slice(at, at + group)
        scaled = rms_scale(gated[:, cut]) * inner_gain[:, cut]
        inner[:, cut] = scaled.astype(BF16)
    wait(1)
    partial[...] = f32_dot(inner[...], mixer_out[...]).astype(BF16)
    for c in range(lanes // CHUNK):
        cut = chunk(c)
        pltpu.make_async_copy(held.at[:, cut], state_out.at[:, cut], out_sem.at[c]).wait()


def mix_heads(
    stream, mixer_gain, gate_proj, input_proj, state_maps, step_proj, step_bias, decay_rate,
    input_taps, map_taps, input_past, map_past, head_state, skip_gain, inner_gain,
    expert_ids, expert_weight, mixer_out,
):
    row_count = stream.shape[0]
    heads, lanes = head_state.shape[1:]
    channels = gate_proj.shape[1]
    flat = row_count * heads
    loads = (
        stream, mixer_gain[None, :], expert_ids.T, expert_weight.T,
        gate_proj, input_proj, state_maps, step_proj.T,
        input_taps, map_taps, input_past.transpose(1, 0, 2),
        map_past.transpose(0, 2, 1, 3).reshape(-1, map_past.shape[3]), inner_gain[None, :], mixer_out,
    )
    vmem = pl.BlockSpec(memory_space=pltpu.VMEM)
    smem = pl.BlockSpec(memory_space=pltpu.SMEM)
    any_space = pl.BlockSpec(memory_space=pl.ANY)
    dma = pltpu.SemaphoreType.DMA
    wide = pltpu.VMEM((flat, 2 * HEAD), F32)
    partial, state_new, note = pl.pallas_call(
        mix_kernel,
        out_shape=(
            jax.ShapeDtypeStruct((row_count, mixer_out.shape[1]), BF16),
            jax.ShapeDtypeStruct((flat, lanes), F32),
            jax.ShapeDtypeStruct((2 * TOP_K, -(-row_count // 128) * 128), F32),
        ),
        in_specs=[smem] * 3 + [any_space] * (LOADS + 1),
        out_specs=(vmem, any_space, vmem),
        scratch_shapes=[pltpu.VMEM(x.shape, x.dtype) for x in loads] + [
            pltpu.VMEM((row_count, channels), BF16),
            pltpu.VMEM((flat, lanes), F32),
            pltpu.VMEM((flat, 4 * HEAD), BF16),
            wide, wide, wide, wide,
            pltpu.VMEM((4 * HEAD, lanes), BF16), pltpu.VMEM((lanes, 2 * HEAD), F32),
            dma((LOADS,)), dma((lanes // CHUNK,)), dma((lanes // CHUNK,)),
        ],
        compiler_params=pltpu.CompilerParams(vmem_limit_bytes=60 * 1024 * 1024),
        name="mix",
    )(step_bias, decay_rate, skip_gain, *loads, head_state.reshape(flat, lanes))
    return partial, state_new.reshape(row_count, heads, lanes), note


class Place:
    def __init__(self, ep_count):
        self.side, self.line = grid_of(ep_count)
        self.ep = lax.axis_index("ep")
        self.core = lax.axis_index("tp")
        self.col = self.ep % self.side
        self.row = (self.ep // self.side) % self.side
        self.z = self.ep // (self.side * self.side)

    def ahead(self, db, da, core=None):
        core = self.core if core is None else core
        a = (self.row * (1 - core) + self.col * core + da) % self.side
        b = (self.col * (1 - core) + self.row * core + db) % self.side
        return a * (1 - core) + b * core, b * (1 - core) + a * core

    def near(self, db, da, dz):
        row, col = self.ahead(db, da)
        z = (self.z + dz) % self.line
        return {"ep": (z * self.side + row) * self.side + col, "tp": self.core}

    def plane(self, db, da):
        row, col = self.ahead(db, da)
        return row * self.side + col

    def partners(self):
        side = range(1, self.side)
        return (
            [self.near(db, da, 0) for db in range(self.side) for da in side]
            + [self.near(d, 0, 0) for d in side]
            + [self.near(0, 0, d) for d in range(1, self.line)]
        )

    def spot(self, db, da, dz):
        return self.plane(db, da) * self.line + (self.z + dz) % self.line

    def sibling(self):
        return {"ep": self.ep, "tp": 1 - self.core}

    def z_order(self):
        last = self.line - 1
        up = (2 * self.z < self.line).astype(jnp.int32)
        at = self.z * up + (last - self.z) * (1 - up)
        order = []
        for i in range(last):
            to = i + (at <= i).astype(jnp.int32)
            order.append(((2 * up - 1) * (to - at)) % self.line)
        return order


def greet(targets):
    barrier = pltpu.get_barrier_semaphore()
    for target in targets:
        pl.semaphore_signal(barrier, inc=1, device_id=target, device_id_type=MESH)
    return lambda: pl.semaphore_wait(barrier, len(targets))


def ffn_kernel(ep_count, *refs):
    (
        partial_in, stream_in, gain_in, note_in, mix_in, dense_gate, dense_up, dense_down,
        expert_gate, expert_up, expert_down, out,
        stream, gain, mix, info, gate_w, up_w, down_w, wide_gate, wide_up, wide_down,
        partial, other, hidden, every, notes, acts, rows, act, dense, own, give, take, share,
        total, from_b, from_a, from_z, from_d,
        load_sem, swap_sem, note_send, note_recv, link_send, link_recv, core_send, core_recv,
        weight_sem, act_send, act_recv, give_sem, sum_send, recv_b, recv_a, recv_z, recv_d,
    ) = refs
    place = Place(ep_count)
    side, line = place.side, place.line
    core, me = place.core, place.ep
    row_count, width = stream.shape
    half = width // 2
    units = dense_gate.shape[0]
    part = row_count // 2
    span = line * row_count
    slots = line * CAP
    my_rows = pl.ds(pl.multiple_of(core * part, part), part)
    my_half = pl.ds(pl.multiple_of(core * half, half), half)
    greeted = greet([place.sibling()] + place.partners())
    sends = []

    def load(at, src, dst):
        copy = pltpu.make_async_copy(src, dst, load_sem.at[at])
        copy.start()
        return copy

    def send(src, dst, send_sem, recv_sem, target):
        copy = pltpu.make_async_remote_copy(
            src_ref=src, dst_ref=dst, send_sem=send_sem, recv_sem=recv_sem,
            device_id=target, device_id_type=MESH,
        )
        copy.start()
        sends.append(copy)
        return copy

    def landed(ref, sem):
        pltpu.make_async_copy(ref, ref, sem).wait()

    here = place.spot(0, 0, 0)
    first_loads = [
        load(0, partial_in, partial), load(1, stream_in, stream), load(2, gain_in, gain),
        load(3, note_in, notes.at[here]),
    ]
    dense_loads = [
        load(4, dense_gate, gate_w.at[core]), load(5, dense_up, up_w.at[core]),
        load(6, dense_down, down_w), load(7, mix_in, mix),
    ]
    first_loads[0].wait()
    greeted()
    swap = send(partial, other, swap_sem.at[0], swap_sem.at[1], place.sibling())
    expert_loads = [
        load(8, expert_gate, wide_gate), load(9, expert_up, wide_up),
        load(10, expert_down, wide_down),
    ]
    for copy in first_loads[1:]:
        copy.wait()
    swap.wait_recv()
    middle = stream[...].astype(F32) + (partial[...].astype(F32) + other[...].astype(F32))
    hidden[...] = middle
    every[here] = (rms_scale(middle) * gain[...]).astype(BF16)

    def slot(db, da, dz):
        return ((db % side) * side + da % side) * line + dz % line

    def block(off):
        return every.at[place.spot(*off), my_rows]

    used = [0]

    def pass_on(off, step):
        there = slot(*(o - s for o, s in zip(off, step)))
        note = notes.at[place.spot(*off)]
        send(note, note, note_send.at[used[0]], note_recv.at[there], place.near(*step))
        send(
            block(off), block(off), link_send.at[used[0]], link_recv.at[there], place.near(*step)
        )
        used[0] += 1

    def arrived(off):
        at = slot(*off)
        landed(notes.at[place.spot(*off)], note_recv.at[at])
        landed(block(off), link_recv.at[at])
        send(block(off), block(off), core_send.at[at], core_recv.at[at], place.sibling())

    zs = [0] + place.z_order()
    for dz in zs[1:]:
        pass_on((0, 0, 0), (0, 0, dz))
    for i, (src, dst) in enumerate(((dense_gate, gate_w), (dense_up, up_w))):
        send(
            src, dst.at[core], weight_sem.at[2 * i], weight_sem.at[2 * i + 1], place.sibling()
        )
    def straight(i):
        return i >= line - STRAIGHT_OUT

    def a_stage(i):
        for da in range(1, side):
            arrived((0, da, zs[i]))
            for d in range(1, 1 if straight(i) else side):
                pass_on((0, da, zs[i]), (d, 0, 0))

    for i, dz in enumerate(zs):
        if i:
            arrived((0, 0, dz))
        for d in range(1, side):
            pass_on((0, 0, dz), (0, d, 0))
        for d in range(1, side):
            pass_on((0, 0, dz), (d, 0, 0))
        if straight(i):
            for d in range(1, side):
                for da in range(1, side):
                    pass_on((0, 0, dz), (d, da, 0))
        if i:
            a_stage(i - 1)
    a_stage(line - 1)

    def planes_of(db):
        return [(db, da) for da in range(side)]

    def group(at, size):
        return pl.ds(pl.multiple_of(at * size, size), size)

    for i, dst in enumerate((gate_w, up_w)):
        dense_loads[i].wait()
        landed(dst.at[1 - core], weight_sem.at[2 * i + 1])

    def dense_in(planes):
        tall = len(planes) * line * part
        seen = jnp.concatenate(
            [every[group(place.plane(*at), line), my_rows].reshape(-1, width) for at in planes],
            axis=0,
        )

        def product(weights):
            return dot_by_rows(seen[:, :half], weights[0]) + dot_by_rows(
                seen[:, half:], weights[1]
            )

        value = (silu(product(gate_w)) * product(up_w)).astype(BF16)
        value = value.reshape(len(planes), line, part, units)
        for i, at in enumerate(planes):
            theirs = acts.at[group(place.plane(*at), line), my_rows]
            acts[group(place.plane(*at), line), my_rows] = value[i]
            k = at[0] * side + at[1]
            send(theirs, theirs, act_send.at[k], act_recv.at[k], place.sibling())

    dense_in(planes_of(0))
    for dz in zs:
        for da in range(side):
            for db in range(1, side):
                arrived((db, da, dz))
    for db in range(1, side):
        dense_in(planes_of(db))
    lanes = notes.shape[2]
    expert = (me // (ep_count // EXPERTS)).astype(F32)
    named = [
        (notes[:, TOP_K + k, :] == expert) & (iota((ep_count, lanes), 1) < row_count)
        for k in range(TOP_K)
    ]
    hits = functools.reduce(jnp.logical_or, named)
    before = iota((lanes, lanes), 0) < iota((lanes, lanes), 1)
    rank = f32_dot(
        jnp.where(hits, 1.0, 0.0).astype(BF16), jnp.where(before, 1.0, 0.0).astype(BF16)
    )
    rank = jnp.where(hits, rank + 1.0, 0.0).astype(BF16)
    weight = sum(jnp.where(named[k], notes[:, k, :], 0.0) for k in range(TOP_K))
    lay = iota((lanes, span), 0) == iota((lanes, span), 1) % row_count
    lay = jnp.where(lay, 1.0, 0.0).astype(BF16)
    chip = iota((ep_count, span), 0)
    for k, parts in enumerate(([rank], parts_of(weight, 3))):
        laid = sum(f32_dot(piece, lay) for piece in parts[::-1])
        for at in range(side * side):
            mine = chip == at * line + iota((ep_count, span), 1) // row_count
            info[k, at] = jnp.sum(jnp.where(mine, laid, 0.0), axis=0, keepdims=True)

    def matches(at):
        slot_id = iota((slots, span), 0)
        row_id = iota((slots, span), 1)
        hit = (slot_id // CAP == row_id // row_count) & (
            (slot_id % CAP + 1).astype(F32) == info[0, at]
        )
        return hit, info[1, at]

    planes = [(db, da) for db in range(side) for da in range(side)]
    for db, da in planes:
        at = place.plane(db, da)
        for i, dz in enumerate(zs):
            if db or da or i:
                theirs = every.at[place.spot(db, da, dz), other_rows(core, part)]
                landed(theirs, core_recv.at[slot(da, db, dz)])
        hit, _ = matches(at)
        pick = jnp.where(hit, 1.0, 0.0).astype(BF16)
        seen = every[group(at, line)].reshape(span, width)
        rows[group(at, slots), :] = f32_dot(pick, seen).astype(BF16)

    for copy in expert_loads:
        copy.wait()
    deep = expert_gate.shape[1]
    for at in range(0, deep, TILE):
        cut = slice(at, min(at + TILE, deep))
        gated = silu(f32_dot(rows[...], wide_gate[:, cut]))
        act[:, cut] = (gated * f32_dot(rows[...], wide_up[:, cut])).astype(BF16)
    scale = []
    for at in range(side * side):
        hit, weight = matches(at)
        scale.append(jnp.sum(jnp.where(hit, weight, 0.0), axis=1, keepdims=True))
    scale = jnp.concatenate(scale, axis=0)

    def results(first, at):
        cut = pl.ds(pl.multiple_of(first * half + at, TILE), TILE)
        return f32_dot(act[...], wide_down[:, cut]) * scale

    for at in range(0, half, TILE):
        give[:, at : at + TILE] = results(1 - core, at).astype(BF16)
    send(give, take, give_sem.at[0], give_sem.at[1], place.sibling())
    for at in range(0, half, TILE):
        own[:, at : at + TILE] = results(core, at)

    dense_loads[2].wait()
    dense_loads[3].wait()
    mixed = jax.nn.sigmoid(mix[...])

    def dense_out(db, da):
        at = place.plane(db, da)
        theirs = acts.at[group(at, line), other_rows(core, part)]
        landed(theirs, act_recv.at[da * side + db])
        seen = acts[group(at, line)].reshape(span, units)
        dense[group(at, span), :] = f32_dot(seen, down_w[...]) * mixed

    for db in range(1, side):
        for da in range(side):
            dense_out(db, da)
    landed(take, give_sem.at[1])
    share[...] = (own[...] + take[...].astype(F32)).astype(BF16)

    def result(db, da):
        at = place.plane(db, da)
        hit, _ = matches(at)
        pick = jnp.where(hit, 1.0, 0.0).T.astype(BF16)
        back = f32_dot(pick, share[group(at, slots), :])
        dense[group(at, span), :] = dense[group(at, span), :] + back

    order = zs[::-1]
    used[0] = 0

    def block_of(off):
        return dense[group(place.spot(*off), row_count), :]

    def give_to(value, dst, sem, step):
        at = used[0]
        used[0] += 1
        total[at] = value.astype(BF16)
        send(total.at[at], dst, sum_send.at[at], sem, place.near(*step))

    def add(value, ref, sem):
        landed(ref, sem)
        return value + ref[...].astype(F32)

    das = list(range(1, side)) + [0]
    for da in das:
        for db in range(1, side):
            result(db, da)
    for i, dz in enumerate(order):
        for da in das:
            for db in range(1, side):
                value = block_of((db, da, dz))
                if da and i < STRAIGHT_BACK:
                    to = (db - 1, da - 1, dz)
                    give_to(value, from_d.at[to], recv_d.at[to], (db, da, 0))
                    continue
                give_to(
                    value, from_b.at[db - 1, da, dz], recv_b.at[db - 1, da, dz], (db, 0, 0)
                )
    for da in das:
        dense_out(0, da)
        result(0, da)

    def after_b(da, i):
        dz = order[i]
        value = block_of((0, da, dz))
        for d in range(1, 1 if da and i < STRAIGHT_BACK else side):
            value = add(value, from_b.at[d - 1, da, dz], recv_b.at[d - 1, da, dz])
        return value

    def a_sums(i):
        dz = order[i]
        for da in range(1, side):
            give_to(after_b(da, i), from_a.at[da - 1, dz], recv_a.at[da - 1, dz], (0, da, 0))

    def after_a(i):
        dz = order[i]
        value = after_b(0, i)
        for d in range(1, side):
            value = add(value, from_a.at[d - 1, dz], recv_a.at[d - 1, dz])
        if i < STRAIGHT_BACK:
            for to in [(d, da, dz) for d in range(side - 1) for da in range(side - 1)]:
                value = add(value, from_d.at[to], recv_d.at[to])
        return value

    a_sums(0)
    for i, dz in enumerate(order[:-1]):
        a_sums(i + 1)
        give_to(after_a(i), from_z.at[dz - 1], recv_z.at[dz - 1], (0, 0, dz))
    value = hidden[:, my_half] + after_a(line - 1)
    for dz in zs[1:]:
        value = add(value, from_z.at[line - dz - 1], recv_z.at[line - dz - 1])
    out[...] = value.astype(out.dtype)
    for copy in sends:
        copy.wait_send()


def other_rows(core, part):
    return pl.ds(pl.multiple_of((1 - core) * part, part), part)


def ffn(
    partial, stream, gain, note, mix, dense_gate, dense_up, dense_down,
    expert_gate, expert_up, expert_down,
):
    ep_count = lax.axis_size("ep")
    side, line = grid_of(ep_count)
    row_count, width = stream.shape
    half = width // 2
    units = dense_gate.shape[0]
    deep = expert_gate.shape[1]
    slots = ep_count * CAP
    more = max(side - 1, 1)
    block = (row_count, half)
    vmem = pl.BlockSpec(memory_space=pltpu.VMEM)
    any_space = pl.BlockSpec(memory_space=pl.ANY)
    dma = pltpu.SemaphoreType.DMA

    def half_words(*shape):
        return pltpu.VMEM(shape, BF16)

    def words(*shape):
        return pltpu.VMEM(shape, F32)

    return pl.pallas_call(
        functools.partial(ffn_kernel, ep_count),
        out_shape=jax.ShapeDtypeStruct(block, BF16),
        in_specs=[any_space] * 11,
        out_specs=vmem,
        scratch_shapes=[
            half_words(row_count, width), words(1, width), words(1, half),
            words(2, side * side, 1, line * row_count),
            half_words(2, units, half), half_words(2, units, half), half_words(units, half),
            half_words(width, deep), half_words(width, deep), half_words(deep, width),
            half_words(row_count, width), half_words(row_count, width), words(row_count, width),
            half_words(ep_count, row_count, width), words(ep_count, *note.shape),
            half_words(ep_count, row_count, units),
            half_words(slots, width), half_words(slots, deep),
            words(ep_count * row_count, half),
            words(slots, half), half_words(slots, half), half_words(slots, half),
            half_words(slots, half),
            half_words(ep_count, *block), half_words(more, side, line, *block),
            half_words(more, line, *block), half_words(max(line - 1, 1), *block),
            half_words(more, more, line, *block),
            dma((11,)), dma((2,)), dma((ep_count,)), dma((ep_count,)),
            dma((ep_count,)), dma((ep_count,)), dma((ep_count,)), dma((ep_count,)),
            dma((4,)), dma((side * side,)), dma((side * side,)), dma((2,)),
            dma((ep_count,)), dma((more, side, line)), dma((more, line)),
            dma((max(line - 1, 1),)), dma((more, more, line)),
        ],
        compiler_params=pltpu.CompilerParams(
            collective_id=1, has_side_effects=True, vmem_limit_bytes=60 * 1024 * 1024
        ),
        name="ffn",
    )(
        partial, stream, gain, note, mix, dense_gate, dense_up, dense_down,
        expert_gate, expert_up, expert_down,
    )


def local(
    stream, mixer_gain, gate_proj, input_proj, state_maps, step_proj, step_bias, decay_rate,
    input_taps, map_taps, input_past, map_past, head_state, skip_gain, inner_gain, mixer_out,
    channel_gain, expert_ids, expert_weight, expert_gate, expert_up, expert_down,
    dense_gate, dense_up, dense_down, dense_mix,
):
    partial, state_out, note = mix_heads(
        stream, mixer_gain, gate_proj, input_proj, state_maps, step_proj, step_bias, decay_rate,
        input_taps, map_taps, input_past, map_past, head_state, skip_gain, inner_gain,
        expert_ids, expert_weight, mixer_out,
    )
    updated = ffn(
        partial, stream, channel_gain[None, :], note, dense_mix[None, :],
        dense_gate.T, dense_up.T, dense_down, expert_gate, expert_up, expert_down,
    )
    return (updated, state_out)


def solution(mesh):
    placed = (
        P("ep", None),
        P(),
        P(None, "tp"),
        P(None, "tp"),
        P(None, None, "tp"),
        P(None, "tp"),
        P("tp"),
        P("tp"),
        P(None, "tp"),
        P(None, None, "tp"),
        P("ep", None, "tp"),
        P("ep", None, None, "tp"),
        P("ep", "tp", None),
        P("tp"),
        P("tp"),
        P("tp", None),
        P(),
        P("ep", None),
        P("ep", None),
        P(None, ("ep", "tp")),
        P(None, ("ep", "tp")),
        P(("ep", "tp"), None),
        P("tp", "ep"),
        P("tp", "ep"),
        P("ep", "tp"),
        P("tp"),
    )
    return jax.shard_map(
        local,
        mesh=mesh,
        in_specs=placed,
        out_specs=(P("ep", "tp"), P("ep", "tp", None)),
        check_vma=False,
    )
```
